128 devices in a mesh: sp: 16 (over z, x), tp: 8 (over y, core).
Axes of the slice: x: 4, y: 4, z: 4, core: 2. Of those that a mesh axis runs over, the one named last changes fastest.
Arguments:
- query_small: bfloat16 [12288, 1024], P('sp', 'tp'), may hold values from -18 to 18
- key_small: bfloat16 [12288, 1024], P('sp', 'tp'), may hold values from -6 to 6
- value_small: bfloat16 [12288, 1024], P('sp', 'tp'), may hold values from -6 to 6
- offset_small: bfloat16 [16, 12288], P('tp', 'sp'), may hold values from -25 to 0
- query_large: bfloat16 [12288, 1024], P('sp', 'tp'), may hold values from -18 to 18
- key_large: bfloat16 [12288, 1024], P('sp', 'tp'), may hold values from -6 to 6
- value_large: bfloat16 [12288, 1024], P('sp', 'tp'), may hold values from -6 to 6
- offset_large: bfloat16 [8, 12288], P('tp', 'sp'), may hold values from -25 to 0
- out_small: bfloat16 [1024, 2048], P('tp'), may hold values from -0.125 to 0.125
- out_large: bfloat16 [1024, 2048], P('tp'), may hold values from -0.125 to 0.125
- residual: bfloat16 [12288, 2048], P(('sp', 'tp')), may hold values from -1.1953125 to 1.1953125
- norm_gain: bfloat16 [2048], replicated, may hold values from 0.099609375 to 1.8984375
- gate_weight: bfloat16 [2048, 5632], P('sp', 'tp'), may hold values from -0.125 to 0.125
- up_weight: bfloat16 [2048, 5632], P('sp', 'tp'), may hold values from -0.125 to 0.125
- down_weight: bfloat16 [5632, 2048], P('tp', 'sp'), may hold values from -0.078125 to 0.078125
Outputs:
- layer_out: bfloat16 [12288, 2048], P(('sp', 'tp'))
The draws below stay inside these ranges and needn't reach their ends.
All inputs are finite; a program needn't handle non-finite values.
Results may differ from the reference program's by a relative error of at most 0.023.
Values may be sent and summed in bfloat16 or wider, within the bound.
No kernel may reach another device: no remote copies, remote signals or barrier semaphores. Data moves between devices by JAX's collectives and lax.ppermute only.
A program may use at most 128 MiB of HBM per device.

```python
import math
import jax
import jax.numpy as jnp
from jax import lax

D = 2048
HEADS_SMALL = 16
SMALL_DIM = 64
HEADS_LARGE = 8
LARGE_DIM = 128
FF = 5632
TOK_DEV = 768
SEQUENCE_LENGTH = 12288
N_TP = 8


def draw_offsets(key, head_count_list):
    random_keys = jax.random.split(key, 7)
    share = 0.5
    quick = jax.random.uniform(random_keys[0], (head_count_list,)) < share
    slow_base = math.log(0.35 / SEQUENCE_LENGTH) - 4.5 + jax.random.uniform(random_keys[1], (head_count_list,), minval=-0.5, maxval=0.5)
    quick_base = -8.4 + jax.random.uniform(random_keys[2], (head_count_list,), minval=-0.5, maxval=0.5)
    baseline_output = jnp.where(quick, quick_base, slow_base)
    position_shifts = jax.random.uniform(random_keys[3], (head_count_list, SEQUENCE_LENGTH // TOK_DEV), minval=-0.7, maxval=0.7)
    position_shifts = jnp.repeat(position_shifts, TOK_DEV, axis=1)
    approximate_output = jax.random.uniform(random_keys[4], (head_count_list, SEQUENCE_LENGTH), minval=-0.5, maxval=0.5)
    sample_spots = jax.random.randint(random_keys[5], (head_count_list, 3), 0, SEQUENCE_LENGTH)
    token_places = jnp.arange(SEQUENCE_LENGTH, dtype=jnp.int32)
    sample_draw = jnp.any(token_places[None, :, None] == sample_spots[:, None, :], axis=2)
    sample_draw_value = jax.random.uniform(random_keys[6], (head_count_list, SEQUENCE_LENGTH), minval=-1.5, maxval=-0.5)
    return jnp.where(sample_draw, sample_draw_value, baseline_output[:, None] + position_shifts + approximate_output).astype(jnp.float32)


def draw_offset_small(key, part):
    return draw_offsets(jax.random.fold_in(key, 11), HEADS_SMALL).astype(jnp.bfloat16)


def draw_offset_large(key, part):
    return draw_offsets(jax.random.fold_in(key, 23), HEADS_LARGE).astype(jnp.bfloat16)


def level_of(rng, extent, shards, least, largest):
    def one(dim, parts):
        steps = jax.random.uniform(jax.random.fold_in(jax.random.fold_in(rng, 6), dim), (parts,), jnp.float32, least / len(shards), largest / len(shards))
        return jnp.repeat(jnp.exp(steps), extent[dim] // parts).reshape((-1,) + (1,) * (len(extent) - dim - 1))

    factor_of = one(*shards[0])
    for cut in shards[1:]:
        factor_of = factor_of * one(*cut)
    return factor_of


def normal_values(rng, extent, width, limit, pieces=(), kind=jnp.bfloat16):
    result = width * jax.random.normal(rng, extent, jnp.float32)
    if pieces:
        result = result * level_of(rng, extent, pieces, -0.22, 0.18)
    return jnp.clip(result, -limit, limit).astype(kind)


def setup_inputs(seed: int = 0) -> dict:
    seeds = jax.random.split(jax.random.key(seed), 16)
    query_small = normal_values(seeds[0], (SEQUENCE_LENGTH, HEADS_SMALL * SMALL_DIM), 3.0, 18.0, ((0, 16), (1, 8)))
    key_small = normal_values(seeds[1], (SEQUENCE_LENGTH, HEADS_SMALL * SMALL_DIM), 1.0, 6.0, ((0, 16), (1, 8)))
    value_small = normal_values(seeds[2], (SEQUENCE_LENGTH, HEADS_SMALL * SMALL_DIM), 1.0, 6.0, ((0, 16), (1, 8)))
    offset_small = draw_offset_small(jax.random.fold_in(seeds[15], 71), 0)
    query_large = normal_values(seeds[4], (SEQUENCE_LENGTH, HEADS_LARGE * LARGE_DIM), 3.0, 18.0, ((0, 16), (1, 8)))
    key_large = normal_values(seeds[5], (SEQUENCE_LENGTH, HEADS_LARGE * LARGE_DIM), 1.0, 6.0, ((0, 16), (1, 8)))
    value_large = normal_values(seeds[6], (SEQUENCE_LENGTH, HEADS_LARGE * LARGE_DIM), 1.0, 6.0, ((0, 16), (1, 8)))
    offset_large = draw_offset_large(jax.random.fold_in(seeds[15], 71), 0)
    out_small = normal_values(seeds[8], (HEADS_SMALL * SMALL_DIM, D), (HEADS_SMALL * SMALL_DIM + HEADS_LARGE * LARGE_DIM) ** -0.5, 0.125, ((0, 8),))
    out_large = normal_values(seeds[9], (HEADS_LARGE * LARGE_DIM, D), (HEADS_SMALL * SMALL_DIM + HEADS_LARGE * LARGE_DIM) ** -0.5, 0.125, ((0, 8),))
    residual = normal_values(seeds[10], (SEQUENCE_LENGTH, D), 0.2, 1.1953125, ((0, 128),))
    norm_gain = jnp.clip(1.0 + 0.18 * jax.random.normal(seeds[11], (D,), jnp.float32), 0.099609375, 1.8984375).astype(jnp.bfloat16)
    gate_weight = normal_values(seeds[12], (D, FF), D ** -0.5, 0.125, ((0, 16), (1, 8)))
    up_weight = normal_values(seeds[13], (D, FF), D ** -0.5, 0.125, ((0, 16), (1, 8)))
    down_weight = normal_values(seeds[14], (FF, D), FF ** -0.5, 0.078125, ((0, 8), (1, 16)))
    return {"query_small": query_small, "key_small": key_small, "value_small": value_small, "offset_small": offset_small, "query_large": query_large, "key_large": key_large, "value_large": value_large, "offset_large": offset_large, "out_small": out_small, "out_large": out_large, "residual": residual, "norm_gain": norm_gain, "gate_weight": gate_weight, "up_weight": up_weight, "down_weight": down_weight}


def stick_group(query, random_keys, values, offset, head_depth):
    head_count_list = offset.shape[0]

    def per_head(args):
        head_query, head_keys, head_values, head_offset = args
        key_pos = jnp.arange(SEQUENCE_LENGTH, dtype=jnp.int32)

        def per_block(first_row):
            block_query = lax.dynamic_slice_in_dim(head_query, first_row, TOK_DEV, 0)
            logits = jnp.dot(block_query, head_keys.T, preferred_element_type=jnp.float32) * head_depth ** (-0.5)
            logits = logits + head_offset.astype(jnp.float32)[None, :]
            query_pos = first_row + jnp.arange(TOK_DEV, dtype=jnp.int32)
            before = key_pos[None, :] < query_pos[:, None]
            fail_all = jax.nn.log_sigmoid(-logits)
            log_pass = logits + fail_all
            log_fail = jnp.where(before, fail_all, 0.0)
            suffix = lax.cumsum(log_fail, axis=1, reverse=True) - log_fail
            weights = jnp.where(before, jnp.exp(log_pass + suffix), 0.0).astype(jnp.bfloat16)
            return jnp.dot(weights, head_values, preferred_element_type=jnp.float32).astype(jnp.bfloat16)
        starts = jnp.arange(SEQUENCE_LENGTH // TOK_DEV, dtype=jnp.int32) * TOK_DEV
        return lax.map(per_block, starts).reshape(SEQUENCE_LENGTH, head_depth)

    def split_heads(flat):
        return flat.reshape(SEQUENCE_LENGTH, head_count_list, head_depth).transpose(1, 0, 2)
    mixed = lax.map(per_head, (split_heads(query), split_heads(random_keys), split_heads(values), offset))
    return mixed.transpose(1, 0, 2).reshape(SEQUENCE_LENGTH, head_count_list * head_depth)

def rounded(value):
    return lax.optimization_barrier(value.astype(jnp.bfloat16)).astype(jnp.float32)

def reference(query_small, key_small, value_small, offset_small, query_large, key_large, value_large, offset_large, out_small, out_large, residual, norm_gain, gate_weight, up_weight, down_weight):
    mixed_small = stick_group(query_small, key_small, value_small, offset_small, SMALL_DIM)
    mixed_large = stick_group(query_large, key_large, value_large, offset_large, LARGE_DIM)
    small_run = HEADS_SMALL * SMALL_DIM // N_TP
    large_run = HEADS_LARGE * LARGE_DIM // N_TP
    total = jnp.zeros((SEQUENCE_LENGTH, D), jnp.float32)
    for group in range(N_TP):
        part = jnp.dot(mixed_small[:, group * small_run:(group + 1) * small_run], out_small[group * small_run:(group + 1) * small_run], preferred_element_type=jnp.float32)
        part = part + jnp.dot(mixed_large[:, group * large_run:(group + 1) * large_run], out_large[group * large_run:(group + 1) * large_run], preferred_element_type=jnp.float32)
        total = total + rounded(part)
    stream = residual.astype(jnp.float32) + rounded(total)
    scale = lax.rsqrt(lax.optimization_barrier(jnp.mean(stream * stream, axis=-1, keepdims=True)) + 1e-06)
    normed = (stream * scale * norm_gain.astype(jnp.float32)).astype(jnp.bfloat16)
    gate = jnp.dot(normed, gate_weight, preferred_element_type=jnp.float32)
    upper = jnp.dot(normed, up_weight, preferred_element_type=jnp.float32)
    hidden = (jax.nn.silu(gate) * upper).astype(jnp.bfloat16)
    hidden_run = FF // N_TP
    summed = jnp.zeros((SEQUENCE_LENGTH, D), jnp.float32)
    for group in range(N_TP):
        part = jnp.dot(hidden[:, group * hidden_run:(group + 1) * hidden_run], down_weight[group * hidden_run:(group + 1) * hidden_run], preferred_element_type=jnp.float32)
        summed = summed + rounded(part)
    return (stream + rounded(summed)).astype(jnp.bfloat16)
```

```python
import functools

import jax
import jax.numpy as jnp
import numpy as np
from jax import lax
from jax.experimental import pallas as pl
from jax.experimental.pallas import tpu as pltpu
from jax.sharding import PartitionSpec as P

LOG2E = 1.4426950408889634
CEILING = 30.0
BLOCK = 768
HALF = 384
ROWS = 784
LANES = 256
FOLD = 3
CHUNK = 128
SCALES = (64**-0.5 * LOG2E, 64**-0.5 * LOG2E, 128**-0.5 * LOG2E)


def attention_chunk(q_ref, kv_ref, tri, acc, carry, row, head, shift):
    col = 0 if head < 2 else 256
    rows = pl.ds(row, CHUNK)
    q = q_ref[0, head, rows, :]
    es, ds, values = [], [], []
    for c in range(FOLD):
        keys = kv_ref[0, c * LANES : (c + 1) * LANES, col : col + 128]
        x = lax.dot_general(q, keys, (((1,), (1,)), ((), ())), preferred_element_type=jnp.float32)
        at = BLOCK + 2 * head + c // 2
        offset = kv_ref[0, at : at + 1, (c % 2) * LANES : (c % 2 + 1) * LANES].astype(jnp.float32)
        x = x * SCALES[head] + offset * LOG2E
        e = jnp.exp2(jnp.minimum(x, CEILING))
        if shift is not None:
            t = lax.broadcasted_iota(jnp.int32, (CHUNK, LANES), 0) + (row + shift)
            s = lax.broadcasted_iota(jnp.int32, (CHUNK, LANES), 1) * FOLD + c
            e = jnp.where(s < t, e, 0.0)
        es.append(e)
        ds.append(1.0 + e)
    log_fail = -jnp.log2(ds[0] * ds[1] * ds[2])
    small = log_fail.astype(jnp.bfloat16)
    later = jnp.dot(small, tri, preferred_element_type=jnp.float32)
    before = carry[head, rows, :]
    scale = jnp.exp2(later + log_fail + before[:, :1])
    total = later[:, :1] + small[:, :1].astype(jnp.float32)
    carry[head, rows, :] = before + total
    result = acc[head, rows, :]
    for c in range(FOLD):
        weights = (es[c] * scale).astype(jnp.bfloat16)
        values = kv_ref[0, c * LANES : (c + 1) * LANES, col + 128 : col + 256]
        result = result + jnp.dot(weights, values, preferred_element_type=jnp.float32)
        if c + 1 < FOLD:
            scale = scale * ds[c]
    acc[head, rows, :] = result


def attention_body(table, q_ref, kv_ref, tri_ref, out_ref, acc, carry):
    step = pl.program_id(0)
    first = table[2, step] == 1

    @pl.when(first)
    def _():
        acc[...] = jnp.zeros_like(acc)
        carry[...] = jnp.zeros_like(carry)

    tri = tri_ref[...]

    def sweep(shift):
        def one(i, _):
            row = pl.multiple_of(i * CHUNK, CHUNK)
            for head in range(3):
                attention_chunk(q_ref, kv_ref, tri, acc, carry, row, head, shift)
            return 0

        lax.fori_loop(0, HALF // CHUNK, one, 0)

    @pl.when(first)
    def _():
        sweep(table[3, step])

    @pl.when(jnp.logical_not(first))
    def _():
        sweep(None)

    @pl.when(table[4, step] == 1)
    def _():
        low = lax.broadcasted_iota(jnp.int32, (HALF, 128), 1) < 64
        out_ref[0, :, :128] = jnp.where(low, acc[0], acc[1]).astype(jnp.bfloat16)
        out_ref[0, :, 128:] = acc[2].astype(jnp.bfloat16)


def attention(table, queries, kv, steps):
    tri = jnp.asarray(np.tril(np.ones((LANES, LANES)), -1), jnp.bfloat16)
    return pl.pallas_call(
        attention_body,
        grid_spec=pltpu.PrefetchScalarGridSpec(
            num_scalar_prefetch=1,
            grid=(steps,),
            in_specs=[
                pl.BlockSpec((1, 3, HALF, 128), lambda i, t: (t[0, i], 0, 0, 0)),
                pl.BlockSpec((1, ROWS, 512), lambda i, t: (t[1, i], 0, 0)),
                pl.BlockSpec((LANES, LANES), lambda i, t: (0, 0)),
            ],
            out_specs=pl.BlockSpec((1, HALF, 256), lambda i, t: (t[0, i], 0, 0)),
            scratch_shapes=[
                pltpu.VMEM((3, HALF, 128), jnp.float32),
                pltpu.VMEM((3, HALF, 128), jnp.float32),
            ],
        ),
        out_shape=jax.ShapeDtypeStruct((2, HALF, 256), jnp.bfloat16),
        compiler_params=pltpu.CompilerParams(
            dimension_semantics=("arbitrary",), vmem_limit_bytes=48 * 2**20
        ),
        name="stick_attention",
    )(table, queries, kv, tri)


def step_table(index, blocks):
    steps = jnp.arange(blocks + 1, dtype=jnp.int32)
    high = 2 * blocks - 1 - index
    count = high // 2 + 1
    on_high = steps < count
    half = jnp.where(on_high, high, index)
    key = jnp.where(on_high, high // 2 - steps, index // 2 - (steps - count))
    first = (steps == 0) | (steps == count)
    last = key == 0
    rows = [jnp.where(on_high, 1, 0), key, first, (half % 2) * HALF, last]
    return jnp.stack([r.astype(jnp.int32) for r in rows])


def zigzag_pairs(blocks, back):
    first, second = [], []
    for i in range(blocks):
        for pairs, h in ((first, 2 * i), (second, 2 * i + 1)):
            to = h if h < blocks else 2 * blocks - 1 - h
            pairs.append((to, i) if back else (i, to))
    return first, second


def packed_keys(key_small, value_small, offset_small, key_large, value_large, offset_large):
    rows = jnp.concatenate([key_small, value_small, key_large, value_large], axis=1)
    rows = rows.reshape(LANES, FOLD, 512).transpose(1, 0, 2).reshape(BLOCK, 512)
    offsets = jnp.concatenate([offset_small, offset_large], axis=0)
    offsets = offsets.reshape(3, LANES, FOLD).transpose(0, 2, 1).reshape(3, BLOCK)
    offsets = jnp.pad(offsets, ((0, 0), (0, 1024 - BLOCK))).reshape(6, 512)
    offsets = jnp.pad(offsets, ((0, ROWS - BLOCK - 6), (0, 0)))
    return jnp.concatenate([rows, offsets], axis=0)


def rms_norm(stream, gain):
    scale = lax.rsqrt(jnp.mean(stream * stream, axis=-1, keepdims=True) + 1e-06)
    return (stream * scale * gain.astype(jnp.float32)).astype(jnp.bfloat16)


def on_device(
    query_small,
    key_small,
    value_small,
    offset_small,
    query_large,
    key_large,
    value_large,
    offset_large,
    out_small,
    out_large,
    residual,
    norm_gain,
    gate_weight,
    up_weight,
    down_weight,
):
    blocks = lax.axis_size("sp")
    index = lax.axis_index("sp")
    kv = packed_keys(key_small, value_small, offset_small, key_large, value_large, offset_large)
    kv = lax.all_gather(kv, "sp", axis=0)
    gate_up = lax.all_gather(
        jnp.concatenate([gate_weight, up_weight], axis=1), "sp", axis=0, tiled=True
    )
    down = lax.all_gather(down_weight, "sp", axis=0)

    queries = jnp.concatenate([query_small, query_large], axis=1)
    first, second = zigzag_pairs(blocks, False)
    one = lax.ppermute(queries[:HALF], "sp", first)
    two = lax.ppermute(queries[HALF:], "sp", second)
    even = index % 2 == 0
    low, high = jnp.where(even, one, two), jnp.where(even, two, one)
    both = jnp.stack([low, high])
    lane = lax.broadcasted_iota(jnp.int32, (1, 1, 128), 2) < 64
    zero = jnp.zeros((), jnp.bfloat16)
    heads = jnp.stack(
        [
            jnp.where(lane, both[:, :, :128], zero),
            jnp.where(lane, zero, both[:, :, :128]),
            both[:, :, 128:],
        ],
        axis=1,
    )
    mixed = attention(step_table(index, blocks), heads, kv, blocks + 1)
    back_first, back_second = zigzag_pairs(blocks, True)
    one = jnp.where(even, mixed[0], mixed[1])
    two = jnp.where(even, mixed[1], mixed[0])
    mixed = jnp.concatenate(
        [lax.ppermute(one, "sp", back_first), lax.ppermute(two, "sp", back_second)], axis=0
    )
    part = jnp.dot(
        mixed, jnp.concatenate([out_small, out_large], axis=0), preferred_element_type=jnp.float32
    ).astype(jnp.bfloat16)
    tp = lax.axis_size("tp")
    arrived = lax.all_to_all(
        part.reshape(tp, -1, part.shape[1]), "tp", split_axis=0, concat_axis=0, tiled=True
    )
    attended = arrived.astype(jnp.float32).sum(axis=0).astype(jnp.bfloat16)
    stream = residual.astype(jnp.float32) + attended.astype(jnp.float32)
    normed = rms_norm(stream, norm_gain)
    normed_rows = lax.all_gather(normed, "tp", axis=0, tiled=True)
    width = gate_weight.shape[1]
    gate = jnp.dot(normed_rows, gate_up[:, :width], preferred_element_type=jnp.float32)
    upper = jnp.dot(normed_rows, gate_up[:, width:], preferred_element_type=jnp.float32)
    hidden = (jax.nn.silu(gate) * upper).astype(jnp.bfloat16)
    down_full = jnp.moveaxis(down, 0, 1).reshape(width, -1)
    summed = lax.psum_scatter(
        jnp.dot(hidden, down_full, preferred_element_type=jnp.float32).astype(jnp.bfloat16),
        "tp",
        scatter_dimension=0,
        tiled=True,
    )
    return (stream + summed.astype(jnp.float32)).astype(jnp.bfloat16)


def solution(mesh):
    return jax.shard_map(
        on_device,
        mesh=mesh,
        in_specs=(
            P("sp", "tp"),
            P("sp", "tp"),
            P("sp", "tp"),
            P("tp", "sp"),
            P("sp", "tp"),
            P("sp", "tp"),
            P("sp", "tp"),
            P("tp", "sp"),
            P("tp", None),
            P("tp", None),
            P(("sp", "tp"), None),
            P(),
            P("sp", "tp"),
            P("sp", "tp"),
            P("tp", "sp"),
        ),
        out_specs=P(("sp", "tp"), None),
        check_vma=False,
    )
```

```python
import jax
import jax.numpy as jnp
import numpy as np
from jax import lax
from jax.experimental import pallas as pl
from jax.experimental.pallas import tpu as pltpu
from jax.sharding import Mesh, PartitionSpec as P

LOG2E = 1.4426950408889634
CEILING = 30.0
BLOCK = 768
HALF = 384
ROWS = 784
LANES = 256
FOLD = 3
SCALES = (64**-0.5 * LOG2E, 64**-0.5 * LOG2E, 128**-0.5 * LOG2E)
SP = ("z", "x")
TP = ("y", "c")


def attention_head(q_ref, kv_ref, tri, acc, carry, odds, weights, head, shift):
    col = 0 if head < 2 else 256
    for c in range(FOLD):
        keys = kv_ref[0, c * LANES : (c + 1) * LANES, col : col + 128]
        at = BLOCK + 2 * head + c // 2
        offset = kv_ref[0, at : at + 1, (c % 2) * LANES : (c % 2 + 1) * LANES].astype(jnp.float32)
        x = lax.dot_general(
            q_ref[0, head], keys, (((1,), (1,)), ((), ())), preferred_element_type=jnp.float32
        )
        e = jnp.exp2(jnp.minimum(x * SCALES[head] + offset * LOG2E, CEILING))
        if shift is not None:
            t = lax.broadcasted_iota(jnp.int32, (HALF, LANES), 0) + shift
            s = lax.broadcasted_iota(jnp.int32, (HALF, LANES), 1) * FOLD + c
            e = jnp.where(s < t, e, 0.0)
        odds[head, c] = e
    log_fail = -jnp.log2((1.0 + odds[head, 0]) * (1.0 + odds[head, 1]) * (1.0 + odds[head, 2]))
    small = log_fail.astype(jnp.bfloat16)
    later = jnp.dot(small, tri, preferred_element_type=jnp.float32)
    before = carry[head]
    scale = jnp.exp2(later + log_fail + before[:, :1])
    carry[head] = before + (later[:, :1] + small[:, :1].astype(jnp.float32))
    for c in range(FOLD):
        e = odds[head, c]
        weights[head, :, c * LANES : (c + 1) * LANES] = (e * scale).astype(jnp.bfloat16)
        if c + 1 < FOLD:
            scale = scale * (1.0 + e)
    values = kv_ref[0, :BLOCK, col + 128 : col + 256]
    acc[head] = acc[head] + jnp.dot(weights[head], values, preferred_element_type=jnp.float32)


def attention_body(table, q_ref, kv_ref, tri_ref, out_ref, acc, carry, odds, weights):
    step = pl.program_id(0)
    first = table[2, step] == 1

    @pl.when(first)
    def _():
        acc[...] = jnp.zeros_like(acc)
        carry[...] = jnp.zeros_like(carry)

    tri = tri_ref[...]

    def sweep(shift):
        for head in range(3):
            attention_head(q_ref, kv_ref, tri, acc, carry, odds, weights, head, shift)

    @pl.when(first)
    def _():
        sweep(table[3, step])

    @pl.when(jnp.logical_not(first))
    def _():
        sweep(None)

    @pl.when(table[4, step] == 1)
    def _():
        low = lax.broadcasted_iota(jnp.int32, (HALF, 128), 1) < 64
        out_ref[0, :, :128] = jnp.where(low, acc[0], acc[1]).astype(jnp.bfloat16)
        out_ref[0, :, 128:] = acc[2].astype(jnp.bfloat16)


def attention(table, queries, kv, steps):
    tri = jnp.asarray(np.tril(np.ones((LANES, LANES)), -1), jnp.bfloat16)
    return pl.pallas_call(
        attention_body,
        grid_spec=pltpu.PrefetchScalarGridSpec(
            num_scalar_prefetch=1,
            grid=(steps,),
            in_specs=[
                pl.BlockSpec((1, 3, HALF, 128), lambda i, t: (t[0, i], 0, 0, 0)),
                pl.BlockSpec((1, ROWS, 512), lambda i, t: (t[1, i], 0, 0)),
                pl.BlockSpec((LANES, LANES), lambda i, t: (0, 0)),
            ],
            out_specs=pl.BlockSpec((1, HALF, 256), lambda i, t: (t[0, i], 0, 0)),
            scratch_shapes=[
                pltpu.VMEM((3, HALF, 128), jnp.float32),
                pltpu.VMEM((3, HALF, 128), jnp.float32),
                pltpu.VMEM((3, FOLD, HALF, LANES), jnp.float32),
                pltpu.VMEM((3, HALF, BLOCK), jnp.bfloat16),
            ],
        ),
        out_shape=jax.ShapeDtypeStruct((2, HALF, 256), jnp.bfloat16),
        compiler_params=pltpu.CompilerParams(
            dimension_semantics=("arbitrary",), vmem_limit_bytes=32 * 2**20
        ),
        name="stick_attention",
    )(table, queries, kv, tri)


def step_table(index, blocks):
    steps = jnp.arange(blocks + 1, dtype=jnp.int32)
    count = index + 1
    own = steps < count
    key = jnp.where(own, index - steps, blocks - 1 - index - (steps - count))
    first = (steps == 0) | (steps == count)
    rows = [jnp.where(own, 0, 1), key, first, jnp.where(own, 0, HALF), key == 0]
    return jnp.stack([r.astype(jnp.int32) for r in rows])


def packed_keys(key_small, value_small, offset_small, key_large, value_large, offset_large):
    rows = jnp.concatenate([key_small, value_small, key_large, value_large], axis=1)
    rows = rows.reshape(LANES, FOLD, 512).transpose(1, 0, 2).reshape(BLOCK, 512)
    offsets = jnp.concatenate([offset_small, offset_large], axis=0)
    offsets = offsets.reshape(3, LANES, FOLD).transpose(0, 2, 1).reshape(3, BLOCK)
    offsets = jnp.pad(offsets, ((0, 0), (0, 1024 - BLOCK))).reshape(6, 512)
    offsets = jnp.pad(offsets, ((0, ROWS - BLOCK - 6), (0, 0)))
    return jnp.concatenate([rows, offsets], axis=0)


def mlp_body(place, *refs):
    (ma, mb, na, nb, ra, rb, gain, o_own, o_other, w_hbm) = refs[:10]
    own_out, mine_out, theirs_out = refs[10:13]
    rows, normed, out_w, w, sems = refs[13:]
    step = pl.program_id(0)
    core = place[1]
    copies = [
        pltpu.make_async_copy(o_own, out_w.at[0:1024], sems.at[0]),
        pltpu.make_async_copy(o_other, out_w.at[1024:2048], sems.at[1]),
        pltpu.make_async_copy(w_hbm, w, sems.at[2]),
    ]

    @pl.when(step == 0)
    def _():
        for copy in copies:
            copy.start()

    rows[:192, :1024] = ma[0]
    rows[192:, :1024] = mb[0]
    rows[:192, 1024:] = na[0]
    rows[192:, 1024:] = nb[0]

    @pl.when(step == 0)
    def _():
        copies[0].wait()
        copies[1].wait()

    part = jnp.dot(rows[...], out_w[...], preferred_element_type=jnp.float32)
    attended = part.astype(jnp.bfloat16).astype(jnp.float32)
    kept = jnp.concatenate([ra[0], rb[0]], axis=0).astype(jnp.float32)
    stream = kept + attended
    scale = lax.rsqrt(jnp.mean(stream * stream, axis=-1, keepdims=True) + 1e-06)
    normed[...] = (stream * scale * gain[...].astype(jnp.float32)).astype(jnp.bfloat16)

    @pl.when(step == 0)
    def _():
        own_out[...] = jnp.where(core == 0, stream[0:96], stream[96:192])
        copies[2].wait()

    both = jnp.dot(normed[...], w[:, :1408], preferred_element_type=jnp.float32)
    gate, upper = both[:, :704], both[:, 704:]
    hidden = (gate / (1.0 + jnp.exp(-gate)) * upper).astype(jnp.bfloat16)
    down = lax.dot_general(
        hidden, w[:, 1408:], (((1,), (1,)), ((), ())), preferred_element_type=jnp.float32
    )
    for k in range(2):
        one, two = down[192 * k : 192 * k + 96], down[192 * k + 96 : 192 * k + 192]
        mine_out[k] = jnp.where(core == 0, one, two).astype(jnp.bfloat16)
        theirs_out[k] = jnp.where(core == 0, two, one).astype(jnp.bfloat16)


def mlp(place, m_own, m_other, kept, gain, o_own, o_other, w):
    def at(k):
        return lambda g, p: ((p[0] + 2 * g + k) % 4, 0, 0)

    m_own, m_other = m_own.reshape(4, 192, 1024), m_other.reshape(4, 192, 1024)
    return pl.pallas_call(
        mlp_body,
        grid_spec=pltpu.PrefetchScalarGridSpec(
            num_scalar_prefetch=1,
            grid=(2,),
            in_specs=[
                pl.BlockSpec((1, 192, 1024), at(0)),
                pl.BlockSpec((1, 192, 1024), at(1)),
                pl.BlockSpec((1, 192, 1024), at(0)),
                pl.BlockSpec((1, 192, 1024), at(1)),
                pl.BlockSpec((1, 192, 2048), at(0)),
                pl.BlockSpec((1, 192, 2048), at(1)),
                pl.BlockSpec((1, 2048), lambda g, p: (0, 0)),
                pl.BlockSpec(memory_space=pl.ANY),
                pl.BlockSpec(memory_space=pl.ANY),
                pl.BlockSpec(memory_space=pl.ANY),
            ],
            out_specs=[
                pl.BlockSpec((96, 2048), lambda g, p: (0, 0)),
                pl.BlockSpec((2, 96, 2048), lambda g, p: (g, 0, 0)),
                pl.BlockSpec((2, 96, 2048), lambda g, p: (g, 0, 0)),
            ],
            scratch_shapes=[
                pltpu.VMEM((HALF, 2048), jnp.bfloat16),
                pltpu.VMEM((HALF, 2048), jnp.bfloat16),
                pltpu.VMEM((2048, 2048), jnp.bfloat16),
                pltpu.VMEM((2048, 2112), jnp.bfloat16),
                pltpu.SemaphoreType.DMA((3,)),
            ],
        ),
        out_shape=[
            jax.ShapeDtypeStruct((96, 2048), jnp.float32),
            jax.ShapeDtypeStruct((4, 96, 2048), jnp.bfloat16),
            jax.ShapeDtypeStruct((4, 96, 2048), jnp.bfloat16),
        ],
        compiler_params=pltpu.CompilerParams(
            dimension_semantics=("arbitrary",), vmem_limit_bytes=58 * 2**20
        ),
        name="project_norm_mlp",
    )(place, m_own, m_own, m_other, m_other, kept, kept, gain, o_own, o_other, w)


def ring(k):
    return [(i, (i + k) % 4) for i in range(4)]


def swapped(a):
    return lax.ppermute(a, "c", [(0, 1), (1, 0)])


def ring_gather(a, axis, dim):
    h = a.shape[0] // 2
    before = lax.ppermute(a, axis, ring(1))
    after = lax.ppermute(a, axis, ring(3))
    top = lax.ppermute(before[:h], axis, ring(1))
    bottom = lax.ppermute(after[h:], axis, ring(3))
    opposite = jnp.concatenate([top, bottom], axis=0)
    if dim is None:
        return jnp.stack([a, after, opposite, before])
    return jnp.concatenate([a, after, opposite, before], axis=dim)


def on_device(
    query_small,
    key_small,
    value_small,
    offset_small,
    query_large,
    key_large,
    value_large,
    offset_large,
    out_small,
    out_large,
    residual,
    norm_gain,
    gate_weight,
    up_weight,
    down_weight,
):
    blocks = lax.axis_size(SP)
    index = lax.axis_index(SP)
    y, core = lax.axis_index("y"), lax.axis_index("c")
    kv = packed_keys(key_small, value_small, offset_small, key_large, value_large, offset_large)
    kv = lax.all_gather(kv, SP, axis=0)
    w = lax.all_gather(
        jnp.concatenate([gate_weight, up_weight, down_weight.T], axis=1), SP, axis=0, tiled=True
    )

    queries = jnp.concatenate([query_small, query_large], axis=1)
    mirror = [(i, blocks - 1 - i) for i in range(blocks)]
    both = jnp.stack([queries[:HALF], lax.ppermute(queries[HALF:], SP, mirror)])
    lane = lax.broadcasted_iota(jnp.int32, (1, 1, 128), 2) < 64
    zero = jnp.zeros((), jnp.bfloat16)
    heads = jnp.stack(
        [
            jnp.where(lane, both[:, :, :128], zero),
            jnp.where(lane, zero, both[:, :, :128]),
            both[:, :, 128:],
        ],
        axis=1,
    )

    o_own = ring_gather(jnp.concatenate([out_small, out_large], axis=0), "y", 0)
    o_other = swapped(o_own)
    r_own = ring_gather(residual, "y", None)
    r_other = swapped(r_own)
    kept = jnp.stack(
        [jnp.where(core == 0, r_own, r_other), jnp.where(core == 0, r_other, r_own)], axis=1
    ).reshape(4, 192, 2048)
    kept = lax.dynamic_slice_in_dim(jnp.concatenate([kept, kept], axis=0), (4 - y) % 4, 4, 0)

    kv, heads, o_own, o_other, kept = lax.optimization_barrier(
        (kv, heads, o_own, o_other, kept)
    )
    mixed = attention(step_table(index, blocks), heads, kv, blocks + 1)
    mixed = jnp.concatenate([mixed[0], lax.ppermute(mixed[1], SP, mirror)], axis=0)
    m_own = ring_gather(mixed, "y", 1)
    m_other = swapped(m_own)
    place = jnp.stack([y, core]).astype(jnp.int32)
    stream, mine, theirs = mlp(
        place, m_own, m_other, kept, norm_gain.reshape(1, -1), o_own, o_other, w
    )
    f32 = jnp.float32
    pair = (mine.astype(f32) + swapped(theirs).astype(f32)).astype(jnp.bfloat16)
    h = pair.shape[1] // 2
    after = lax.ppermute(pair[1], "y", ring(1))
    before = lax.ppermute(pair[3], "y", ring(3))
    top = lax.ppermute(pair[2, :h], "y", ring(2))
    bottom = lax.ppermute(pair[2, h:], "y", ring(-2))
    opposite = jnp.concatenate([top, bottom], axis=0)
    summed = pair[0].astype(f32) + after.astype(f32) + before.astype(f32) + opposite.astype(f32)
    return (stream + summed.astype(jnp.bfloat16).astype(f32)).astype(jnp.bfloat16)


def solution(mesh):
    named = Mesh(mesh.devices.reshape(4, 4, 4, 2), SP + TP)
    return jax.shard_map(
        on_device,
        mesh=named,
        in_specs=(
            P(SP, TP),
            P(SP, TP),
            P(SP, TP),
            P(TP, SP),
            P(SP, TP),
            P(SP, TP),
            P(SP, TP),
            P(TP, SP),
            P(TP, None),
            P(TP, None),
            P(SP + TP, None),
            P(),
            P(SP, TP),
            P(SP, TP),
            P(TP, SP),
        ),
        out_specs=P(SP + TP, None),
        check_vma=False,
    )
```

```python
import jax
import jax.numpy as jnp
import numpy as np
from jax import lax
from jax.experimental import pallas as pl
from jax.experimental.pallas import tpu as pltpu
from jax.sharding import Mesh, PartitionSpec as P


LOG2E = 1.4426950408889634
CEILING = 30.0
BLOCK = 768
RUN = 384
ROWS = 784
LANES = 256
FOLD = 3
SCALES = (64**-0.5 * LOG2E, 64**-0.5 * LOG2E, 128**-0.5 * LOG2E)
SP = ("z", "x")
TP = ("y", "c")


def attention_body(table, q_ref, kv_ref, off_ref, tri_ref, out_ref, totals, *scratch):
    odds, weights, later, total_columns, first_head = scratch
    step = pl.program_id(0)
    kind = table[step]
    key = step % 4
    low = lax.broadcasted_iota(jnp.int32, (RUN, 128), 1) < 64
    zero = jnp.zeros((), jnp.bfloat16)

    def odds_of(slot, head, row, diagonal):
        rows = pl.ds(row, RUN)
        col, queries = (0, slice(0, 128)) if head < 2 else (256, slice(128, 256))
        q = q_ref[0, rows, queries]
        if head == 0:
            q = jnp.where(low, q, zero)
        if head == 1:
            q = jnp.where(low, zero, q)
        for c in range(FOLD):
            keys = kv_ref[key, c * LANES : (c + 1) * LANES, col : col + 128]
            x = lax.dot_general(
                q, keys, (((1,), (1,)), ((), ())), preferred_element_type=jnp.float32
            )
            x = x * SCALES[head] + off_ref[key, head, c : c + 1, :]
            e = jnp.exp2(jnp.minimum(x, CEILING))
            if diagonal:
                t = lax.broadcasted_iota(jnp.int32, (RUN, LANES), 0) + row
                s = lax.broadcasted_iota(jnp.int32, (RUN, LANES), 1) * FOLD + c
                e = jnp.where(s < t, e, 0.0)
            odds[slot, c] = e

    def suffix_of(slot, head, row):
        rows = pl.ds(row, RUN)
        log_pass = jnp.log2((1.0 + odds[slot, 0]) * (1.0 + odds[slot, 1]) * (1.0 + odds[slot, 2]))
        short = (-log_pass).astype(jnp.bfloat16)
        after = jnp.dot(short, tri_ref[...], preferred_element_type=jnp.float32)
        later[slot] = after - log_pass
        total = after[:, :1] + short[:, :1].astype(jnp.float32)
        lane = lax.broadcasted_iota(jnp.int32, (RUN, 128), 1)
        total_columns[rows] = jnp.where(lane == step * 3 + head, total, total_columns[rows])

    def mixed_of(slot, head, row):
        rows = pl.ds(row, RUN)
        scale = jnp.exp2(later[slot])
        for c in range(FOLD):
            e = odds[slot, c]
            weights[slot, :, c * LANES : (c + 1) * LANES] = (e * scale).astype(jnp.bfloat16)
            if c + 1 < FOLD:
                scale = scale * (1.0 + e)
        col = 128 if head < 2 else 384
        values = kv_ref[key, :BLOCK, col : col + 128]
        result = jnp.dot(weights[slot], values, preferred_element_type=jnp.float32)
        if head == 0:
            first_head[rows] = result
        elif head == 1:
            out_ref[0, rows, :128] = jnp.where(low, first_head[rows], result).astype(jnp.bfloat16)
        else:
            out_ref[0, rows, 128:] = result.astype(jnp.bfloat16)

    def sweep(runs, diagonal):
        for t in range(len(runs) + 2):
            if t < len(runs):
                odds_of(t % 3, *runs[t], diagonal)
            if 0 <= t - 1 < len(runs):
                suffix_of((t - 1) % 3, *runs[t - 1])
            if 0 <= t - 2:
                mixed_of((t - 2) % 3, *runs[t - 2])

    @pl.when(step == 0)
    def _():
        total_columns[...] = jnp.zeros_like(total_columns)

    @pl.when(kind == 0)
    def _():
        out_ref[...] = jnp.zeros_like(out_ref)

    @pl.when(kind == 1)
    def _():
        sweep([(head, row) for head in range(3) for row in range(0, BLOCK, RUN)], False)

    @pl.when(kind == 2)
    def _():
        def one(i, _):
            sweep([(head, pl.multiple_of(i * RUN, RUN)) for head in range(3)], True)
            return 0

        lax.fori_loop(0, BLOCK // RUN, one, 0)

    @pl.when(step == 15)
    def _():
        totals[...] = jnp.transpose(total_columns[...])[:48]


def attention(kinds, queries, kv, offsets):
    tri = jnp.asarray(np.tril(np.ones((LANES, LANES)), -1), jnp.bfloat16)
    return pl.pallas_call(
        attention_body,
        grid_spec=pltpu.PrefetchScalarGridSpec(
            num_scalar_prefetch=1,
            grid=(16,),
            in_specs=[
                pl.BlockSpec((1, BLOCK, 256), lambda i, t: (i // 4, 0, 0)),
                pl.BlockSpec((4, ROWS, 512), lambda i, t: (0, 0, 0)),
                pl.BlockSpec((4, 3, 4, LANES), lambda i, t: (0, 0, 0, 0)),
                pl.BlockSpec((LANES, LANES), lambda i, t: (0, 0)),
            ],
            out_specs=[
                pl.BlockSpec((1, BLOCK, 256), lambda i, t: (i, 0, 0)),
                pl.BlockSpec((48, BLOCK), lambda i, t: (0, 0)),
            ],
            scratch_shapes=[
                pltpu.VMEM((3, FOLD, RUN, LANES), jnp.float32),
                pltpu.VMEM((3, RUN, BLOCK), jnp.bfloat16),
                pltpu.VMEM((3, RUN, LANES), jnp.float32),
                pltpu.VMEM((BLOCK, 128), jnp.float32),
                pltpu.VMEM((BLOCK, 128), jnp.float32),
            ],
        ),
        out_shape=[
            jax.ShapeDtypeStruct((16, BLOCK, 256), jnp.bfloat16),
            jax.ShapeDtypeStruct((48, BLOCK), jnp.float32),
        ],
        compiler_params=pltpu.CompilerParams(
            dimension_semantics=("arbitrary",), vmem_limit_bytes=40 * 2**20
        ),
        name="stick_attention",
    )(kinds, queries, kv, offsets, tri)


def combine_body(place, outs, t0, t1, t2, t3, part, factors):
    i = pl.program_id(0)
    z, x = place[0], place[1]
    tables = (t0, t1, t2, t3)
    factors[...] = jnp.zeros_like(factors)

    def flag(condition):
        return jnp.where(condition, 1.0, 0.0)

    for head in range(3):
        whole, above = [], []
        for j in range(4):
            rows = [
                tables[k][pl.ds(((i - k + 4) % 4 * 4 + j) * 3 + head, 1), :] for k in range(4)
            ]
            whole.append(rows[0] + rows[1] + rows[2] + rows[3])
            above.append(sum(rows[k] * flag((x + k) % 4 > x) for k in range(1, 4)))
        for j in range(4):
            later = above[j]
            for other in range(4):
                if other != j:
                    later = later + whole[other] * flag((z + other) % 4 > (z + j) % 4)
            factors[j * 3 + head : j * 3 + head + 1, :] = jnp.exp2(later)
    turned = jnp.transpose(factors[...])
    low = lax.broadcasted_iota(jnp.int32, (BLOCK, 128), 1) < 64
    small = large = 0.0
    for j in range(4):
        f = [turned[:, 3 * j + head : 3 * j + head + 1] for head in range(3)]
        small = small + outs[j, :, :128].astype(jnp.float32) * jnp.where(low, f[0], f[1])
        large = large + outs[j, :, 128:].astype(jnp.float32) * f[2]
    part[0, :, :128] = small.astype(jnp.bfloat16)
    part[0, :, 128:] = large.astype(jnp.bfloat16)


def combine(place, outs, tables):
    whole = pl.BlockSpec((48, BLOCK), lambda i, p: (0, 0))
    return pl.pallas_call(
        combine_body,
        grid_spec=pltpu.PrefetchScalarGridSpec(
            num_scalar_prefetch=1,
            grid=(4,),
            in_specs=[pl.BlockSpec((4, BLOCK, 256), lambda i, p: (i, 0, 0))] + [whole] * 4,
            out_specs=pl.BlockSpec((1, BLOCK, 256), lambda i, p: (i, 0, 0)),
            scratch_shapes=[pltpu.VMEM((128, BLOCK), jnp.float32)],
        ),
        out_shape=jax.ShapeDtypeStruct((4, BLOCK, 256), jnp.bfloat16),
        compiler_params=pltpu.CompilerParams(
            dimension_semantics=("arbitrary",), vmem_limit_bytes=24 * 2**20
        ),
        name="combine_key_blocks",
    )(place, outs, *tables)


def balanced(back):
    pairs = []
    for z in range(4):
        for x in range(4):
            chunk = 2 * z + x // 2
            to = 4 * (chunk if chunk < 4 else 7 - chunk) + x
            pairs.append((to, 4 * z + x) if back else (4 * z + x, to))
    return pairs


def tile_kinds(z, x):
    home = np.zeros(16, np.int32)
    for source, to in balanced(False):
        home[to] = source
    ahead = jnp.arange(4, dtype=jnp.int32)
    query = jnp.asarray(home)[4 * z + (x + ahead) % 4]
    key = 4 * ((z + ahead) % 4) + x
    before = (key[None, :] < query[:, None]).astype(jnp.int32)
    same = (key[None, :] == query[:, None]).astype(jnp.int32)
    return (before + 2 * same).reshape(16)


def packed_keys(key_small, value_small, offset_small, key_large, value_large, offset_large):
    rows = jnp.concatenate([key_small, value_small, key_large, value_large], axis=1)
    rows = rows.reshape(LANES, FOLD, 512).transpose(1, 0, 2).reshape(BLOCK, 512)
    offsets = jnp.concatenate([offset_small, offset_large], axis=0)
    offsets = offsets.reshape(3, LANES, FOLD).transpose(0, 2, 1).reshape(3, BLOCK)
    offsets = jnp.pad(offsets, ((0, 0), (0, 1024 - BLOCK))).reshape(6, 512)
    offsets = jnp.pad(offsets, ((0, ROWS - BLOCK - 6), (0, 0)))
    return jnp.concatenate([rows, offsets], axis=0)


def mlp_body(place, *refs):
    (ma, mb, na, nb, r_own, r_other, gain, o_own, o_other, w_hbm) = refs[:10]
    own_out, mine_out, theirs_out = refs[10:13]
    rows, normed, out_w, w, sems = refs[13:]
    step = pl.program_id(0)
    core = place[1]
    copies = [
        pltpu.make_async_copy(o_own, out_w.at[0:1024], sems.at[0]),
        pltpu.make_async_copy(o_other, out_w.at[1024:2048], sems.at[1]),
        pltpu.make_async_copy(w_hbm, w, sems.at[2]),
    ]

    @pl.when(step == 0)
    def _():
        for copy in copies:
            copy.start()

    rows[:192, :1024] = ma[0]
    rows[192:, :1024] = mb[0]
    rows[:192, 1024:] = na[0]
    rows[192:, 1024:] = nb[0]

    @pl.when(step == 0)
    def _():
        copies[0].wait()
        copies[1].wait()

    part = jnp.dot(rows[...], out_w[...], preferred_element_type=jnp.float32)
    attended = part.astype(jnp.bfloat16).astype(jnp.float32)
    kept = []
    for k in range(2):
        mine, theirs = r_own[k].astype(jnp.float32), r_other[k].astype(jnp.float32)
        kept += [jnp.where(core == 0, mine, theirs), jnp.where(core == 0, theirs, mine)]
    kept = jnp.concatenate(kept, axis=0)
    stream = kept + attended
    scale = lax.rsqrt(jnp.mean(stream * stream, axis=-1, keepdims=True) + 1e-06)
    normed[...] = (stream * scale * gain[...].astype(jnp.float32)).astype(jnp.bfloat16)

    @pl.when(step == 0)
    def _():
        own_out[...] = jnp.where(core == 0, stream[0:96], stream[96:192])
        copies[2].wait()

    both = jnp.dot(normed[...], w[:, :1408], preferred_element_type=jnp.float32)
    gate, upper = both[:, :704], both[:, 704:]
    hidden = (gate / (1.0 + jnp.exp(-gate)) * upper).astype(jnp.bfloat16)
    down = lax.dot_general(
        hidden, w[:, 1408:], (((1,), (1,)), ((), ())), preferred_element_type=jnp.float32
    )
    for k in range(2):
        one, two = down[192 * k : 192 * k + 96], down[192 * k + 96 : 192 * k + 192]
        mine_out[k] = jnp.where(core == 0, one, two).astype(jnp.bfloat16)
        theirs_out[k] = jnp.where(core == 0, two, one).astype(jnp.bfloat16)


def mlp(place, m_own, m_other, r_own, r_other, gain, o_own, o_other, w):
    def at(k):
        return lambda g, p: ((p[0] + 2 * g + k) % 4, 0, 0)

    m_own, m_other = m_own.reshape(4, 192, 1024), m_other.reshape(4, 192, 1024)
    return pl.pallas_call(
        mlp_body,
        grid_spec=pltpu.PrefetchScalarGridSpec(
            num_scalar_prefetch=1,
            grid=(2,),
            in_specs=[
                pl.BlockSpec((1, 192, 1024), at(0)),
                pl.BlockSpec((1, 192, 1024), at(1)),
                pl.BlockSpec((1, 192, 1024), at(0)),
                pl.BlockSpec((1, 192, 1024), at(1)),
                pl.BlockSpec((2, 96, 2048), lambda g, p: (g, 0, 0)),
                pl.BlockSpec((2, 96, 2048), lambda g, p: (g, 0, 0)),
                pl.BlockSpec((1, 2048), lambda g, p: (0, 0)),
                pl.BlockSpec(memory_space=pl.ANY),
                pl.BlockSpec(memory_space=pl.ANY),
                pl.BlockSpec(memory_space=pl.ANY),
            ],
            out_specs=[
                pl.BlockSpec((96, 2048), lambda g, p: (0, 0)),
                pl.BlockSpec((2, 96, 2048), lambda g, p: (g, 0, 0)),
                pl.BlockSpec((2, 96, 2048), lambda g, p: (g, 0, 0)),
            ],
            scratch_shapes=[
                pltpu.VMEM((384, 2048), jnp.bfloat16),
                pltpu.VMEM((384, 2048), jnp.bfloat16),
                pltpu.VMEM((2048, 2048), jnp.bfloat16),
                pltpu.VMEM((2048, 2112), jnp.bfloat16),
                pltpu.SemaphoreType.DMA((3,)),
            ],
        ),
        out_shape=[
            jax.ShapeDtypeStruct((96, 2048), jnp.float32),
            jax.ShapeDtypeStruct((4, 96, 2048), jnp.bfloat16),
            jax.ShapeDtypeStruct((4, 96, 2048), jnp.bfloat16),
        ],
        compiler_params=pltpu.CompilerParams(
            dimension_semantics=("arbitrary",), vmem_limit_bytes=58 * 2**20
        ),
        name="project_norm_mlp",
    )(place, m_own, m_own, m_other, m_other, r_own, r_other, gain, o_own, o_other, w)


def ring(k):
    return [(i, (i + k) % 4) for i in range(4)]


def swapped(a):
    return lax.ppermute(a, "c", [(0, 1), (1, 0)])


def ring_gather(a, axis, dim):
    h = a.shape[0] // 2
    before = lax.ppermute(a, axis, ring(1))
    after = lax.ppermute(a, axis, ring(3))
    top = lax.ppermute(before[:h], axis, ring(1))
    bottom = lax.ppermute(after[h:], axis, ring(3))
    opposite = jnp.concatenate([top, bottom], axis=0)
    if dim is None:
        return jnp.stack([a, after, opposite, before])
    return jnp.concatenate([a, after, opposite, before], axis=dim)


def passed_on(before, after, axis):
    h = before.shape[0] // 2
    top = lax.ppermute(before[:h], axis, ring(1))
    bottom = lax.ppermute(after[h:], axis, ring(3))
    return top, bottom


def together(a, before, after, opposite):
    return jnp.stack([a, after, jnp.concatenate(opposite, axis=0), before])


def exchanged(pieces, axis):
    h = pieces.shape[1] // 2
    after = lax.ppermute(pieces[1], axis, ring(1))
    before = lax.ppermute(pieces[3], axis, ring(3))
    top = lax.ppermute(pieces[2, :h], axis, ring(2))
    bottom = lax.ppermute(pieces[2, h:], axis, ring(-2))
    opposite = jnp.concatenate([top, bottom], axis=0).astype(jnp.float32)
    near = pieces[0].astype(jnp.float32) + after.astype(jnp.float32) + before.astype(jnp.float32)
    return near + opposite


def on_device(
    query_small,
    key_small,
    value_small,
    offset_small,
    query_large,
    key_large,
    value_large,
    offset_large,
    out_small,
    out_large,
    residual,
    norm_gain,
    gate_weight,
    up_weight,
    down_weight,
):
    z, x = lax.axis_index("z"), lax.axis_index("x")
    y, core = lax.axis_index("y"), lax.axis_index("c")
    kinds = tile_kinds(z, x)
    queries = jnp.concatenate([query_small, query_large], axis=1)
    kv = packed_keys(key_small, value_small, offset_small, key_large, value_large, offset_large)
    kv, queries = lax.optimization_barrier((kv, queries))
    kv_before = lax.ppermute(kv, "z", ring(1))
    kv_after = lax.ppermute(kv, "z", ring(3))
    queries = lax.ppermute(queries, SP, balanced(False))
    q_before = lax.ppermute(queries, "x", ring(1))
    q_after = lax.ppermute(queries, "x", ring(3))
    w = jnp.concatenate([gate_weight, up_weight, down_weight.T], axis=1)
    q_after, w = lax.optimization_barrier((q_after, w))
    w = lax.all_gather(w, SP, axis=0, tiled=True)
    kv = together(kv, kv_before, kv_after, passed_on(kv_before, kv_after, "z"))
    queries = together(queries, q_before, q_after, passed_on(q_before, q_after, "x"))
    outs_in = jnp.concatenate([out_small, out_large], axis=0)
    o_before = lax.ppermute(outs_in, "y", ring(1))
    o_after = lax.ppermute(outs_in, "y", ring(3))
    offsets = kv[:, BLOCK : BLOCK + 6].reshape(4, 3, 4, LANES).astype(jnp.float32) * LOG2E

    kv, queries, offsets, kinds, o_before, o_after, residual = lax.optimization_barrier(
        (kv, queries, offsets, kinds, o_before, o_after, residual)
    )
    r_before = lax.ppermute(residual, "y", ring(1))
    r_after = lax.ppermute(residual, "y", ring(3))
    o_opposite = passed_on(o_before, o_after, "y")
    outs, totals = attention(kinds, queries, kv, offsets)
    outs, totals, r_before, r_after, o_opposite = lax.optimization_barrier(
        (outs, totals, r_before, r_after, o_opposite)
    )
    o_own = together(outs_in, o_before, o_after, o_opposite).reshape(1024, 2048)
    from_before = lax.ppermute(totals, "x", ring(1))
    from_after = lax.ppermute(totals, "x", ring(3))
    from_opposite = lax.ppermute(totals, "x", ring(2))
    spot = jnp.stack([z, x]).astype(jnp.int32)
    o_other = swapped(o_own)
    r_opposite = passed_on(r_before, r_after, "y")
    r_own = together(residual, r_before, r_after, r_opposite)
    r_other = swapped(r_own)
    part = combine(spot, outs, (totals, from_after, from_opposite, from_before))
    mixed = exchanged(part, "x").astype(jnp.bfloat16)
    mixed = lax.ppermute(mixed, SP, balanced(True))
    m_own = ring_gather(mixed, "y", 1)
    m_other = swapped(m_own)
    place = jnp.stack([y, core]).astype(jnp.int32)
    stream, mine, theirs = mlp(
        place, m_own, m_other, r_own, r_other, norm_gain.reshape(1, -1), o_own, o_other, w
    )
    f32 = jnp.float32
    pair = (mine.astype(f32) + swapped(theirs).astype(f32)).astype(jnp.bfloat16)
    summed = exchanged(pair, "y")
    return (stream + summed.astype(jnp.bfloat16).astype(f32)).astype(jnp.bfloat16)


def solution(mesh):
    named = Mesh(mesh.devices.reshape(4, 4, 4, 2), SP + TP)

    return jax.shard_map(
        on_device,
        mesh=named,
        in_specs=(
            P(SP, TP),
            P(SP, TP),
            P(SP, TP),
            P(TP, SP),
            P(SP, TP),
            P(SP, TP),
            P(SP, TP),
            P(TP, SP),
            P(TP, None),
            P(TP, None),
            P(SP + TP, None),
            P(),
            P(SP, TP),
            P(SP, TP),
            P(TP, SP),
        ),
        out_specs=P(SP + TP, None),
        check_vma=False,
    )
```

```python
import jax
import jax.numpy as jnp
import numpy as np
from jax import lax
from jax.experimental import pallas as pl
from jax.experimental.pallas import tpu as pltpu
from jax.sharding import Mesh, PartitionSpec as P


LOG2E = 1.4426950408889634
CEILING = 30.0
BLOCK = 768
RUN = 384
ROWS = 784
LANES = 256
FOLD = 3
SCALES = (64**-0.5 * LOG2E, 64**-0.5 * LOG2E, 128**-0.5 * LOG2E)
SP = ("z", "x")
TP = ("y", "c")


def attention_body(table, q_ref, kv_ref, off_ref, tri_ref, out_ref, totals, *scratch):
    odds, weights, later, total_columns, first_head = scratch
    step = pl.program_id(0)
    kind = table[step]
    key = step % 4
    low = lax.broadcasted_iota(jnp.int32, (RUN, 128), 1) < 64
    zero = jnp.zeros((), jnp.bfloat16)

    def odds_of(slot, head, row, diagonal):
        rows = pl.ds(row, RUN)
        col, queries = (0, slice(0, 128)) if head < 2 else (256, slice(128, 256))
        q = q_ref[0, rows, queries]
        if head == 0:
            q = jnp.where(low, q, zero)
        if head == 1:
            q = jnp.where(low, zero, q)
        for c in range(FOLD):
            keys = kv_ref[key, c * LANES : (c + 1) * LANES, col : col + 128]
            x = lax.dot_general(
                q, keys, (((1,), (1,)), ((), ())), preferred_element_type=jnp.float32
            )
            x = x * SCALES[head] + off_ref[key, head, c : c + 1, :]
            e = jnp.exp2(jnp.minimum(x, CEILING))
            if diagonal:
                t = lax.broadcasted_iota(jnp.int32, (RUN, LANES), 0) + row
                s = lax.broadcasted_iota(jnp.int32, (RUN, LANES), 1) * FOLD + c
                e = jnp.where(s < t, e, 0.0)
            odds[slot, c] = e

    def suffix_of(slot, head, row):
        rows = pl.ds(row, RUN)
        log_pass = jnp.log2((1.0 + odds[slot, 0]) * (1.0 + odds[slot, 1]) * (1.0 + odds[slot, 2]))
        short = (-log_pass).astype(jnp.bfloat16)
        after = jnp.dot(short, tri_ref[...], preferred_element_type=jnp.float32)
        later[slot] = after - log_pass
        total = after[:, :1] + short[:, :1].astype(jnp.float32)
        lane = lax.broadcasted_iota(jnp.int32, (RUN, 128), 1)
        total_columns[rows] = jnp.where(lane == step * 3 + head, total, total_columns[rows])

    def mixed_of(slot, head, row):
        rows = pl.ds(row, RUN)
        scale = jnp.exp2(later[slot])
        for c in range(FOLD):
            e = odds[slot, c]
            weights[slot, :, c * LANES : (c + 1) * LANES] = (e * scale).astype(jnp.bfloat16)
            if c + 1 < FOLD:
                scale = scale * (1.0 + e)
        col = 128 if head < 2 else 384
        values = kv_ref[key, :BLOCK, col : col + 128]
        result = jnp.dot(weights[slot], values, preferred_element_type=jnp.float32)
        if head == 0:
            first_head[rows] = result
        elif head == 1:
            out_ref[0, rows, :128] = jnp.where(low, first_head[rows], result).astype(jnp.bfloat16)
        else:
            out_ref[0, rows, 128:] = result.astype(jnp.bfloat16)

    def sweep(runs, diagonal):
        for t in range(len(runs) + 2):
            if t < len(runs):
                odds_of(t % 3, *runs[t], diagonal)
            if 0 <= t - 1 < len(runs):
                suffix_of((t - 1) % 3, *runs[t - 1])
            if 0 <= t - 2:
                mixed_of((t - 2) % 3, *runs[t - 2])

    @pl.when(step == 0)
    def _():
        total_columns[...] = jnp.zeros_like(total_columns)

    @pl.when(kind == 0)
    def _():
        out_ref[...] = jnp.zeros_like(out_ref)

    @pl.when(kind == 1)
    def _():
        sweep([(head, row) for head in range(3) for row in range(0, BLOCK, RUN)], False)

    @pl.when(kind == 2)
    def _():
        def one(i, _):
            sweep([(head, pl.multiple_of(i * RUN, RUN)) for head in range(3)], True)
            return 0

        lax.fori_loop(0, BLOCK // RUN, one, 0)

    @pl.when(step == 15)
    def _():
        totals[...] = jnp.transpose(total_columns[...])[:48]


def attention(kinds, queries, kv, offsets):
    tri = jnp.asarray(np.tril(np.ones((LANES, LANES)), -1), jnp.bfloat16)
    return pl.pallas_call(
        attention_body,
        grid_spec=pltpu.PrefetchScalarGridSpec(
            num_scalar_prefetch=1,
            grid=(16,),
            in_specs=[
                pl.BlockSpec((1, BLOCK, 256), lambda i, t: (i // 4, 0, 0)),
                pl.BlockSpec((4, ROWS, 512), lambda i, t: (0, 0, 0)),
                pl.BlockSpec((4, 3, 4, LANES), lambda i, t: (0, 0, 0, 0)),
                pl.BlockSpec((LANES, LANES), lambda i, t: (0, 0)),
            ],
            out_specs=[
                pl.BlockSpec((1, BLOCK, 256), lambda i, t: (i, 0, 0)),
                pl.BlockSpec((48, BLOCK), lambda i, t: (0, 0)),
            ],
            scratch_shapes=[
                pltpu.VMEM((3, FOLD, RUN, LANES), jnp.float32),
                pltpu.VMEM((3, RUN, BLOCK), jnp.bfloat16),
                pltpu.VMEM((3, RUN, LANES), jnp.float32),
                pltpu.VMEM((BLOCK, 128), jnp.float32),
                pltpu.VMEM((BLOCK, 128), jnp.float32),
            ],
        ),
        out_shape=[
            jax.ShapeDtypeStruct((16, BLOCK, 256), jnp.bfloat16),
            jax.ShapeDtypeStruct((48, BLOCK), jnp.float32),
        ],
        compiler_params=pltpu.CompilerParams(
            dimension_semantics=("arbitrary",), vmem_limit_bytes=40 * 2**20
        ),
        name="stick_attention",
    )(kinds, queries, kv, offsets, tri)


def combine_body(place, outs, t0, t1, t2, t3, part, factors):
    i = pl.program_id(0)
    z, x = place[0], place[1]
    tables = (t0, t1, t2, t3)
    factors[...] = jnp.zeros_like(factors)

    def flag(condition):
        return jnp.where(condition, 1.0, 0.0)

    for head in range(3):
        whole, above = [], []
        for j in range(4):
            rows = [
                tables[k][pl.ds(((i - k + 4) % 4 * 4 + j) * 3 + head, 1), :] for k in range(4)
            ]
            whole.append(rows[0] + rows[1] + rows[2] + rows[3])
            above.append(sum(rows[k] * flag((x + k) % 4 > x) for k in range(1, 4)))
        for j in range(4):
            later = above[j]
            for other in range(4):
                if other != j:
                    later = later + whole[other] * flag((z + other) % 4 > (z + j) % 4)
            factors[j * 3 + head : j * 3 + head + 1, :] = jnp.exp2(later)
    turned = jnp.transpose(factors[...])
    low = lax.broadcasted_iota(jnp.int32, (BLOCK, 128), 1) < 64
    small = large = 0.0
    for j in range(4):
        f = [turned[:, 3 * j + head : 3 * j + head + 1] for head in range(3)]
        small = small + outs[j, :, :128].astype(jnp.float32) * jnp.where(low, f[0], f[1])
        large = large + outs[j, :, 128:].astype(jnp.float32) * f[2]
    part[0, :, :128] = small.astype(jnp.bfloat16)
    part[0, :, 128:] = large.astype(jnp.bfloat16)


def combine(place, outs, tables):
    whole = pl.BlockSpec((48, BLOCK), lambda i, p: (0, 0))
    return pl.pallas_call(
        combine_body,
        grid_spec=pltpu.PrefetchScalarGridSpec(
            num_scalar_prefetch=1,
            grid=(4,),
            in_specs=[pl.BlockSpec((4, BLOCK, 256), lambda i, p: (i, 0, 0))] + [whole] * 4,
            out_specs=pl.BlockSpec((1, BLOCK, 256), lambda i, p: (i, 0, 0)),
            scratch_shapes=[pltpu.VMEM((128, BLOCK), jnp.float32)],
        ),
        out_shape=jax.ShapeDtypeStruct((4, BLOCK, 256), jnp.bfloat16),
        compiler_params=pltpu.CompilerParams(
            dimension_semantics=("arbitrary",), vmem_limit_bytes=24 * 2**20
        ),
        name="combine_key_blocks",
    )(place, outs, *tables)


def balanced(back):
    pairs = []
    for z in range(4):
        for x in range(4):
            chunk = 2 * z + x // 2
            to = 4 * (chunk if chunk < 4 else 7 - chunk) + x
            pairs.append((to, 4 * z + x) if back else (4 * z + x, to))
    return pairs


def tile_kinds(z, x):
    home = np.zeros(16, np.int32)
    for source, to in balanced(False):
        home[to] = source
    ahead = jnp.arange(4, dtype=jnp.int32)
    query = jnp.asarray(home)[4 * z + (x + ahead) % 4]
    key = 4 * ((z + ahead) % 4) + x
    before = (key[None, :] < query[:, None]).astype(jnp.int32)
    same = (key[None, :] == query[:, None]).astype(jnp.int32)
    return (before + 2 * same).reshape(16)


def packed_keys(key_small, value_small, offset_small, key_large, value_large, offset_large):
    rows = jnp.concatenate([key_small, value_small, key_large, value_large], axis=1)
    rows = rows.reshape(LANES, FOLD, 512).transpose(1, 0, 2).reshape(BLOCK, 512)
    offsets = jnp.concatenate([offset_small, offset_large], axis=0)
    offsets = offsets.reshape(3, LANES, FOLD).transpose(0, 2, 1).reshape(3, BLOCK)
    offsets = jnp.pad(offsets, ((0, 0), (0, 1024 - BLOCK))).reshape(6, 512)
    offsets = jnp.pad(offsets, ((0, ROWS - BLOCK - 6), (0, 0)))
    return jnp.concatenate([rows, offsets], axis=0)


def mlp_body(place, *refs):
    (ma, mb, na, nb, r_own, r_other, gain, o_own, o_other, w_hbm) = refs[:10]
    own_out, mine_out, theirs_out = refs[10:13]
    rows, normed, out_w, w, sems = refs[13:]
    step = pl.program_id(0)
    core = place[1]
    copies = [
        pltpu.make_async_copy(o_own, out_w.at[0:1024], sems.at[0]),
        pltpu.make_async_copy(o_other, out_w.at[1024:2048], sems.at[1]),
        pltpu.make_async_copy(w_hbm, w, sems.at[2]),
    ]

    @pl.when(step == 0)
    def _():
        for copy in copies:
            copy.start()

    rows[:192, :1024] = ma[0]
    rows[192:, :1024] = mb[0]
    rows[:192, 1024:] = na[0]
    rows[192:, 1024:] = nb[0]

    @pl.when(step == 0)
    def _():
        copies[0].wait()
        copies[1].wait()

    part = jnp.dot(rows[...], out_w[...], preferred_element_type=jnp.float32)
    attended = part.astype(jnp.bfloat16).astype(jnp.float32)
    kept = []
    for k in range(2):
        mine, theirs = r_own[k].astype(jnp.float32), r_other[k].astype(jnp.float32)
        kept += [jnp.where(core == 0, mine, theirs), jnp.where(core == 0, theirs, mine)]
    kept = jnp.concatenate(kept, axis=0)
    stream = kept + attended
    scale = lax.rsqrt(jnp.mean(stream * stream, axis=-1, keepdims=True) + 1e-06)
    normed[...] = (stream * scale * gain[...].astype(jnp.float32)).astype(jnp.bfloat16)

    @pl.when(step == 0)
    def _():
        own_out[...] = jnp.where(core == 0, stream[0:96], stream[96:192])
        copies[2].wait()

    both = jnp.dot(normed[...], w[:, :1408], preferred_element_type=jnp.float32)
    gate, upper = both[:, :704], both[:, 704:]
    hidden = (gate / (1.0 + jnp.exp(-gate)) * upper).astype(jnp.bfloat16)
    down = lax.dot_general(
        hidden, w[:, 1408:], (((1,), (1,)), ((), ())), preferred_element_type=jnp.float32
    )
    for k in range(2):
        one, two = down[192 * k : 192 * k + 96], down[192 * k + 96 : 192 * k + 192]
        mine_out[k] = jnp.where(core == 0, one, two).astype(jnp.bfloat16)
        theirs_out[k] = jnp.where(core == 0, two, one).astype(jnp.bfloat16)


def mlp(place, m_own, m_other, r_own, r_other, gain, o_own, o_other, w):
    def at(k):
        return lambda g, p: ((p[0] + 2 * g + k) % 4, 0, 0)

    m_own, m_other = m_own.reshape(4, 192, 1024), m_other.reshape(4, 192, 1024)
    return pl.pallas_call(
        mlp_body,
        grid_spec=pltpu.PrefetchScalarGridSpec(
            num_scalar_prefetch=1,
            grid=(2,),
            in_specs=[
                pl.BlockSpec((1, 192, 1024), at(0)),
                pl.BlockSpec((1, 192, 1024), at(1)),
                pl.BlockSpec((1, 192, 1024), at(0)),
                pl.BlockSpec((1, 192, 1024), at(1)),
                pl.BlockSpec((2, 96, 2048), lambda g, p: (g, 0, 0)),
                pl.BlockSpec((2, 96, 2048), lambda g, p: (g, 0, 0)),
                pl.BlockSpec((1, 2048), lambda g, p: (0, 0)),
                pl.BlockSpec(memory_space=pl.ANY),
                pl.BlockSpec(memory_space=pl.ANY),
                pl.BlockSpec(memory_space=pl.ANY),
            ],
            out_specs=[
                pl.BlockSpec((96, 2048), lambda g, p: (0, 0)),
                pl.BlockSpec((2, 96, 2048), lambda g, p: (g, 0, 0)),
                pl.BlockSpec((2, 96, 2048), lambda g, p: (g, 0, 0)),
            ],
            scratch_shapes=[
                pltpu.VMEM((384, 2048), jnp.bfloat16),
                pltpu.VMEM((384, 2048), jnp.bfloat16),
                pltpu.VMEM((2048, 2048), jnp.bfloat16),
                pltpu.VMEM((2048, 2112), jnp.bfloat16),
                pltpu.SemaphoreType.DMA((3,)),
            ],
        ),
        out_shape=[
            jax.ShapeDtypeStruct((96, 2048), jnp.float32),
            jax.ShapeDtypeStruct((4, 96, 2048), jnp.bfloat16),
            jax.ShapeDtypeStruct((4, 96, 2048), jnp.bfloat16),
        ],
        compiler_params=pltpu.CompilerParams(
            dimension_semantics=("arbitrary",), vmem_limit_bytes=58 * 2**20
        ),
        name="project_norm_mlp",
    )(place, m_own, m_own, m_other, m_other, r_own, r_other, gain, o_own, o_other, w)


def ring(k):
    return [(i, (i + k) % 4) for i in range(4)]


def swapped(a):
    return lax.ppermute(a, "c", [(0, 1), (1, 0)])


def ring_gather(a, axis, dim):
    h = a.shape[0] // 2
    before = lax.ppermute(a, axis, ring(1))
    after = lax.ppermute(a, axis, ring(3))
    top = lax.ppermute(before[:h], axis, ring(1))
    bottom = lax.ppermute(after[h:], axis, ring(3))
    opposite = jnp.concatenate([top, bottom], axis=0)
    if dim is None:
        return jnp.stack([a, after, opposite, before])
    return jnp.concatenate([a, after, opposite, before], axis=dim)


def passed_on(before, after, axis):
    h = before.shape[0] // 2
    top = lax.ppermute(before[:h], axis, ring(1))
    bottom = lax.ppermute(after[h:], axis, ring(3))
    return top, bottom


def together(a, before, after, opposite):
    return jnp.stack([a, after, jnp.concatenate(opposite, axis=0), before])


def exchanged(pieces, axis):
    h = pieces.shape[1] // 2
    after = lax.ppermute(pieces[1], axis, ring(1))
    before = lax.ppermute(pieces[3], axis, ring(3))
    top = lax.ppermute(pieces[2, :h], axis, ring(2))
    bottom = lax.ppermute(pieces[2, h:], axis, ring(-2))
    opposite = jnp.concatenate([top, bottom], axis=0).astype(jnp.float32)
    near = pieces[0].astype(jnp.float32) + after.astype(jnp.float32) + before.astype(jnp.float32)
    return near + opposite


def on_device(
    query_small,
    key_small,
    value_small,
    offset_small,
    query_large,
    key_large,
    value_large,
    offset_large,
    out_small,
    out_large,
    residual,
    norm_gain,
    gate_weight,
    up_weight,
    down_weight,
):
    z, x = lax.axis_index("z"), lax.axis_index("x")
    y, core = lax.axis_index("y"), lax.axis_index("c")
    kinds = tile_kinds(z, x)
    queries = jnp.concatenate([query_small, query_large], axis=1)
    kv = packed_keys(key_small, value_small, offset_small, key_large, value_large, offset_large)
    kv, queries = lax.optimization_barrier((kv, queries))
    kv_before = lax.ppermute(kv, "z", ring(1))
    kv_after = lax.ppermute(kv, "z", ring(3))
    queries = lax.ppermute(queries, SP, balanced(False))
    q_before = lax.ppermute(queries, "x", ring(1))
    q_after = lax.ppermute(queries, "x", ring(3))
    w = jnp.concatenate([gate_weight, up_weight, down_weight.T], axis=1)
    q_after, w = lax.optimization_barrier((q_after, w))
    w = lax.all_gather(w, SP, axis=0, tiled=True)
    kv = together(kv, kv_before, kv_after, passed_on(kv_before, kv_after, "z"))
    queries = together(queries, q_before, q_after, passed_on(q_before, q_after, "x"))
    outs_in = jnp.concatenate([out_small, out_large], axis=0)
    o_before = lax.ppermute(outs_in, "y", ring(1))
    o_after = lax.ppermute(outs_in, "y", ring(3))
    offsets = kv[:, BLOCK : BLOCK + 6].reshape(4, 3, 4, LANES).astype(jnp.float32) * LOG2E

    outs, totals = attention(kinds, queries, kv, offsets)
    outs, totals, o_before, o_after, residual = lax.optimization_barrier(
        (outs, totals, o_before, o_after, residual)
    )
    r_before = lax.ppermute(residual, "y", ring(1))
    r_after = lax.ppermute(residual, "y", ring(3))
    o_opposite = passed_on(o_before, o_after, "y")
    o_own = together(outs_in, o_before, o_after, o_opposite).reshape(1024, 2048)
    from_before = lax.ppermute(totals, "x", ring(1))
    from_after = lax.ppermute(totals, "x", ring(3))
    from_opposite = lax.ppermute(totals, "x", ring(2))
    spot = jnp.stack([z, x]).astype(jnp.int32)
    o_other = swapped(o_own)
    r_opposite = passed_on(r_before, r_after, "y")
    r_own = together(residual, r_before, r_after, r_opposite)
    r_other = swapped(r_own)
    part = combine(spot, outs, (totals, from_after, from_opposite, from_before))
    mixed = exchanged(part, "x").astype(jnp.bfloat16)
    mixed = lax.ppermute(mixed, SP, balanced(True))
    m_own = ring_gather(mixed, "y", 1)
    m_other = swapped(m_own)
    place = jnp.stack([y, core]).astype(jnp.int32)
    stream, mine, theirs = mlp(
        place, m_own, m_other, r_own, r_other, norm_gain.reshape(1, -1), o_own, o_other, w
    )
    f32 = jnp.float32
    pair = (mine.astype(f32) + swapped(theirs).astype(f32)).astype(jnp.bfloat16)
    summed = exchanged(pair, "y")
    return (stream + summed.astype(jnp.bfloat16).astype(f32)).astype(jnp.bfloat16)


def solution(mesh):
    named = Mesh(mesh.devices.reshape(4, 4, 4, 2), SP + TP)

    return jax.shard_map(
        on_device,
        mesh=named,
        in_specs=(
            P(SP, TP),
            P(SP, TP),
            P(SP, TP),
            P(TP, SP),
            P(SP, TP),
            P(SP, TP),
            P(SP, TP),
            P(TP, SP),
            P(TP, None),
            P(TP, None),
            P(SP + TP, None),
            P(),
            P(SP, TP),
            P(SP, TP),
            P(TP, SP),
        ),
        out_specs=P(SP + TP, None),
        check_vma=False,
    )
```

```python
import jax
import jax.numpy as jnp
import numpy as np
from jax import lax
from jax.experimental import pallas as pl
from jax.experimental.pallas import tpu as pltpu
from jax.sharding import Mesh, PartitionSpec as P


LOG2E = 1.4426950408889634
CEILING = 30.0
BLOCK = 768
RUN = 384
ROWS = 784
LANES = 256
FOLD = 3
SCALES = (64**-0.5 * LOG2E, 64**-0.5 * LOG2E, 128**-0.5 * LOG2E)
SP = ("z", "x")
TP = ("y", "c")


def attention_body(table, q_ref, kv_ref, off_ref, tri_ref, out_ref, totals, *scratch):
    odds, weights, later, total_columns, first_head = scratch
    step = pl.program_id(0)
    kind = table[step]
    key = step % 4
    low = lax.broadcasted_iota(jnp.int32, (RUN, 128), 1) < 64
    zero = jnp.zeros((), jnp.bfloat16)

    def odds_of(slot, head, row, diagonal):
        rows = pl.ds(row, RUN)
        col, queries = (0, slice(0, 128)) if head < 2 else (256, slice(128, 256))
        q = q_ref[0, rows, queries]
        if head == 0:
            q = jnp.where(low, q, zero)
        if head == 1:
            q = jnp.where(low, zero, q)
        for c in range(FOLD):
            keys = kv_ref[key, c * LANES : (c + 1) * LANES, col : col + 128]
            x = lax.dot_general(
                q, keys, (((1,), (1,)), ((), ())), preferred_element_type=jnp.float32
            )
            x = x * SCALES[head] + off_ref[key, head, c : c + 1, :]
            e = jnp.exp2(jnp.minimum(x, CEILING))
            if diagonal:
                t = lax.broadcasted_iota(jnp.int32, (RUN, LANES), 0) + row
                s = lax.broadcasted_iota(jnp.int32, (RUN, LANES), 1) * FOLD + c
                e = jnp.where(s < t, e, 0.0)
            odds[slot, c] = e

    def suffix_of(slot, head, row):
        rows = pl.ds(row, RUN)
        log_pass = jnp.log2((1.0 + odds[slot, 0]) * (1.0 + odds[slot, 1]) * (1.0 + odds[slot, 2]))
        short = (-log_pass).astype(jnp.bfloat16)
        after = jnp.dot(short, tri_ref[...], preferred_element_type=jnp.float32)
        later[slot] = after - log_pass
        total = after[:, :1] + short[:, :1].astype(jnp.float32)
        lane = lax.broadcasted_iota(jnp.int32, (RUN, 128), 1)
        total_columns[rows] = jnp.where(lane == step * 3 + head, total, total_columns[rows])

    def mixed_of(slot, head, row):
        rows = pl.ds(row, RUN)
        scale = jnp.exp2(later[slot])
        for c in range(FOLD):
            e = odds[slot, c]
            weights[slot, :, c * LANES : (c + 1) * LANES] = (e * scale).astype(jnp.bfloat16)
            if c + 1 < FOLD:
                scale = scale * (1.0 + e)
        col = 128 if head < 2 else 384
        values = kv_ref[key, :BLOCK, col : col + 128]
        result = jnp.dot(weights[slot], values, preferred_element_type=jnp.float32)
        if head == 0:
            first_head[rows] = result
        elif head == 1:
            out_ref[0, rows, :128] = jnp.where(low, first_head[rows], result).astype(jnp.bfloat16)
        else:
            out_ref[0, rows, 128:] = result.astype(jnp.bfloat16)

    def sweep(runs, diagonal):
        for t in range(len(runs) + 2):
            if t < len(runs):
                odds_of(t % 3, *runs[t], diagonal)
            if 0 <= t - 1 < len(runs):
                suffix_of((t - 1) % 3, *runs[t - 1])
            if 0 <= t - 2:
                mixed_of((t - 2) % 3, *runs[t - 2])

    @pl.when(step == 0)
    def _():
        total_columns[...] = jnp.zeros_like(total_columns)

    @pl.when(kind == 0)
    def _():
        out_ref[...] = jnp.zeros_like(out_ref)

    @pl.when(kind == 1)
    def _():
        sweep([(head, row) for head in range(3) for row in range(0, BLOCK, RUN)], False)

    @pl.when(kind == 2)
    def _():
        def one(i, _):
            sweep([(head, pl.multiple_of(i * RUN, RUN)) for head in range(3)], True)
            return 0

        lax.fori_loop(0, BLOCK // RUN, one, 0)

    @pl.when(step == 15)
    def _():
        totals[...] = jnp.transpose(total_columns[...])[:48]


def attention(kinds, queries, kv, offsets):
    tri = jnp.asarray(np.tril(np.ones((LANES, LANES)), -1), jnp.bfloat16)
    return pl.pallas_call(
        attention_body,
        grid_spec=pltpu.PrefetchScalarGridSpec(
            num_scalar_prefetch=1,
            grid=(16,),
            in_specs=[
                pl.BlockSpec((1, BLOCK, 256), lambda i, t: (i // 4, 0, 0)),
                pl.BlockSpec((4, ROWS, 512), lambda i, t: (0, 0, 0)),
                pl.BlockSpec((4, 3, 4, LANES), lambda i, t: (0, 0, 0, 0)),
                pl.BlockSpec((LANES, LANES), lambda i, t: (0, 0)),
            ],
            out_specs=[
                pl.BlockSpec((1, BLOCK, 256), lambda i, t: (i, 0, 0)),
                pl.BlockSpec((48, BLOCK), lambda i, t: (0, 0)),
            ],
            scratch_shapes=[
                pltpu.VMEM((3, FOLD, RUN, LANES), jnp.float32),
                pltpu.VMEM((3, RUN, BLOCK), jnp.bfloat16),
                pltpu.VMEM((3, RUN, LANES), jnp.float32),
                pltpu.VMEM((BLOCK, 128), jnp.float32),
                pltpu.VMEM((BLOCK, 128), jnp.float32),
            ],
        ),
        out_shape=[
            jax.ShapeDtypeStruct((16, BLOCK, 256), jnp.bfloat16),
            jax.ShapeDtypeStruct((48, BLOCK), jnp.float32),
        ],
        compiler_params=pltpu.CompilerParams(
            dimension_semantics=("arbitrary",), vmem_limit_bytes=40 * 2**20
        ),
        name="stick_attention",
    )(kinds, queries, kv, offsets, tri)


def combine_body(place, outs, t0, t1, t2, t3, part, factors):
    i = pl.program_id(0)
    z, x = place[0], place[1]
    tables = (t0, t1, t2, t3)
    factors[...] = jnp.zeros_like(factors)

    def flag(condition):
        return jnp.where(condition, 1.0, 0.0)

    for head in range(3):
        whole, above = [], []
        for j in range(4):
            rows = [
                tables[k][pl.ds(((i - k + 4) % 4 * 4 + j) * 3 + head, 1), :] for k in range(4)
            ]
            whole.append(rows[0] + rows[1] + rows[2] + rows[3])
            above.append(sum(rows[k] * flag((x + k) % 4 > x) for k in range(1, 4)))
        for j in range(4):
            later = above[j]
            for other in range(4):
                if other != j:
                    later = later + whole[other] * flag((z + other) % 4 > (z + j) % 4)
            factors[j * 3 + head : j * 3 + head + 1, :] = jnp.exp2(later)
    turned = jnp.transpose(factors[...])
    low = lax.broadcasted_iota(jnp.int32, (BLOCK, 128), 1) < 64
    small = large = 0.0
    for j in range(4):
        f = [turned[:, 3 * j + head : 3 * j + head + 1] for head in range(3)]
        small = small + outs[j, :, :128].astype(jnp.float32) * jnp.where(low, f[0], f[1])
        large = large + outs[j, :, 128:].astype(jnp.float32) * f[2]
    part[0, :, :128] = small.astype(jnp.bfloat16)
    part[0, :, 128:] = large.astype(jnp.bfloat16)


def combine(place, outs, tables):
    whole = pl.BlockSpec((48, BLOCK), lambda i, p: (0, 0))
    return pl.pallas_call(
        combine_body,
        grid_spec=pltpu.PrefetchScalarGridSpec(
            num_scalar_prefetch=1,
            grid=(4,),
            in_specs=[pl.BlockSpec((4, BLOCK, 256), lambda i, p: (i, 0, 0))] + [whole] * 4,
            out_specs=pl.BlockSpec((1, BLOCK, 256), lambda i, p: (i, 0, 0)),
            scratch_shapes=[pltpu.VMEM((128, BLOCK), jnp.float32)],
        ),
        out_shape=jax.ShapeDtypeStruct((4, BLOCK, 256), jnp.bfloat16),
        compiler_params=pltpu.CompilerParams(
            dimension_semantics=("arbitrary",), vmem_limit_bytes=24 * 2**20
        ),
        name="combine_key_blocks",
    )(place, outs, *tables)


def balanced(back):
    pairs = []
    for z in range(4):
        for x in range(4):
            chunk = 2 * z + x // 2
            to = 4 * (chunk if chunk < 4 else 7 - chunk) + x
            pairs.append((to, 4 * z + x) if back else (4 * z + x, to))
    return pairs


def tile_kinds(z, x):
    home = np.zeros(16, np.int32)
    for source, to in balanced(False):
        home[to] = source
    ahead = jnp.arange(4, dtype=jnp.int32)
    query = jnp.asarray(home)[4 * z + (x + ahead) % 4]
    key = 4 * ((z + ahead) % 4) + x
    before = (key[None, :] < query[:, None]).astype(jnp.int32)
    same = (key[None, :] == query[:, None]).astype(jnp.int32)
    return (before + 2 * same).reshape(16)


def packed_keys(key_small, value_small, offset_small, key_large, value_large, offset_large):
    rows = jnp.concatenate([key_small, value_small, key_large, value_large], axis=1)
    rows = rows.reshape(LANES, FOLD, 512).transpose(1, 0, 2).reshape(BLOCK, 512)
    offsets = jnp.concatenate([offset_small, offset_large], axis=0)
    offsets = offsets.reshape(3, LANES, FOLD).transpose(0, 2, 1).reshape(3, BLOCK)
    offsets = jnp.pad(offsets, ((0, 0), (0, 1024 - BLOCK))).reshape(6, 512)
    offsets = jnp.pad(offsets, ((0, ROWS - BLOCK - 6), (0, 0)))
    return jnp.concatenate([rows, offsets], axis=0)


def mlp_body(place, *refs):
    (ma, mb, na, nb, r_own, r_other, gain, o_own, o_other, w_hbm) = refs[:10]
    own_out, mine_out, theirs_out = refs[10:13]
    rows, normed, out_w, w, sems = refs[13:]
    step = pl.program_id(0)
    core = place[1]
    copies = [
        pltpu.make_async_copy(o_own, out_w.at[0:1024], sems.at[0]),
        pltpu.make_async_copy(o_other, out_w.at[1024:2048], sems.at[1]),
        pltpu.make_async_copy(w_hbm, w, sems.at[2]),
    ]

    @pl.when(step == 0)
    def _():
        copies[0].start()
        copies[1].start()

    rows[:192, :1024] = ma[0]
    rows[192:, :1024] = mb[0]
    rows[:192, 1024:] = na[0]
    rows[192:, 1024:] = nb[0]

    @pl.when(step == 0)
    def _():
        copies[0].wait()
        copies[2].start()

    part = jnp.dot(rows[:, :1024], out_w[:1024], preferred_element_type=jnp.float32)

    @pl.when(step == 0)
    def _():
        copies[1].wait()

    part = part + jnp.dot(rows[:, 1024:], out_w[1024:], preferred_element_type=jnp.float32)
    attended = part.astype(jnp.bfloat16).astype(jnp.float32)
    kept = []
    for k in range(2):
        mine, theirs = r_own[k].astype(jnp.float32), r_other[k].astype(jnp.float32)
        kept += [jnp.where(core == 0, mine, theirs), jnp.where(core == 0, theirs, mine)]
    kept = jnp.concatenate(kept, axis=0)
    stream = kept + attended
    scale = lax.rsqrt(jnp.mean(stream * stream, axis=-1, keepdims=True) + 1e-06)
    normed[...] = (stream * scale * gain[...].astype(jnp.float32)).astype(jnp.bfloat16)

    @pl.when(step == 0)
    def _():
        own_out[...] = jnp.where(core == 0, stream[0:96], stream[96:192])
        copies[2].wait()

    both = jnp.dot(normed[...], w[:, :1408], preferred_element_type=jnp.float32)
    gate, upper = both[:, :704], both[:, 704:]
    hidden = (gate / (1.0 + jnp.exp(-gate)) * upper).astype(jnp.bfloat16)
    down = lax.dot_general(
        hidden, w[:, 1408:], (((1,), (1,)), ((), ())), preferred_element_type=jnp.float32
    )
    for k in range(2):
        one, two = down[192 * k : 192 * k + 96], down[192 * k + 96 : 192 * k + 192]
        mine_out[k] = jnp.where(core == 0, one, two).astype(jnp.bfloat16)
        theirs_out[k] = jnp.where(core == 0, two, one).astype(jnp.bfloat16)


def mlp(place, m_own, m_other, r_own, r_other, gain, o_own, o_other, w):
    def at(k):
        return lambda g, p: ((p[0] + 2 * g + k) % 4, 0, 0)

    m_own, m_other = m_own.reshape(4, 192, 1024), m_other.reshape(4, 192, 1024)
    return pl.pallas_call(
        mlp_body,
        grid_spec=pltpu.PrefetchScalarGridSpec(
            num_scalar_prefetch=1,
            grid=(2,),
            in_specs=[
                pl.BlockSpec((1, 192, 1024), at(0)),
                pl.BlockSpec((1, 192, 1024), at(1)),
                pl.BlockSpec((1, 192, 1024), at(0)),
                pl.BlockSpec((1, 192, 1024), at(1)),
                pl.BlockSpec((2, 96, 2048), lambda g, p: (g, 0, 0)),
                pl.BlockSpec((2, 96, 2048), lambda g, p: (g, 0, 0)),
                pl.BlockSpec((1, 2048), lambda g, p: (0, 0)),
                pl.BlockSpec(memory_space=pl.ANY),
                pl.BlockSpec(memory_space=pl.ANY),
                pl.BlockSpec(memory_space=pl.ANY),
            ],
            out_specs=[
                pl.BlockSpec((96, 2048), lambda g, p: (0, 0)),
                pl.BlockSpec((2, 96, 2048), lambda g, p: (g, 0, 0)),
                pl.BlockSpec((2, 96, 2048), lambda g, p: (g, 0, 0)),
            ],
            scratch_shapes=[
                pltpu.VMEM((384, 2048), jnp.bfloat16),
                pltpu.VMEM((384, 2048), jnp.bfloat16),
                pltpu.VMEM((2048, 2048), jnp.bfloat16),
                pltpu.VMEM((2048, 2112), jnp.bfloat16),
                pltpu.SemaphoreType.DMA((3,)),
            ],
        ),
        out_shape=[
            jax.ShapeDtypeStruct((96, 2048), jnp.float32),
            jax.ShapeDtypeStruct((4, 96, 2048), jnp.bfloat16),
            jax.ShapeDtypeStruct((4, 96, 2048), jnp.bfloat16),
        ],
        compiler_params=pltpu.CompilerParams(
            dimension_semantics=("arbitrary",), vmem_limit_bytes=58 * 2**20
        ),
        name="project_norm_mlp",
    )(place, m_own, m_own, m_other, m_other, r_own, r_other, gain, o_own, o_other, w)


def ring(k):
    return [(i, (i + k) % 4) for i in range(4)]


def swapped(a):
    return lax.ppermute(a, "c", [(0, 1), (1, 0)])


def ring_gather(a, axis, dim):
    h = a.shape[0] // 2
    before = lax.ppermute(a, axis, ring(1))
    after = lax.ppermute(a, axis, ring(3))
    top = lax.ppermute(before[:h], axis, ring(1))
    bottom = lax.ppermute(after[h:], axis, ring(3))
    opposite = jnp.concatenate([top, bottom], axis=0)
    if dim is None:
        return jnp.stack([a, after, opposite, before])
    return jnp.concatenate([a, after, opposite, before], axis=dim)


def passed_on(before, after, axis):
    h = before.shape[0] // 2
    top = lax.ppermute(before[:h], axis, ring(1))
    bottom = lax.ppermute(after[h:], axis, ring(3))
    return top, bottom


def together(a, before, after, opposite):
    return jnp.stack([a, after, jnp.concatenate(opposite, axis=0), before])


def exchanged(pieces, axis):
    h = pieces.shape[1] // 2
    after = lax.ppermute(pieces[1], axis, ring(1))
    before = lax.ppermute(pieces[3], axis, ring(3))
    top = lax.ppermute(pieces[2, :h], axis, ring(2))
    bottom = lax.ppermute(pieces[2, h:], axis, ring(-2))
    opposite = jnp.concatenate([top, bottom], axis=0).astype(jnp.float32)
    near = pieces[0].astype(jnp.float32) + after.astype(jnp.float32) + before.astype(jnp.float32)
    return near + opposite


def on_device(
    query_small,
    key_small,
    value_small,
    offset_small,
    query_large,
    key_large,
    value_large,
    offset_large,
    out_small,
    out_large,
    residual,
    norm_gain,
    gate_weight,
    up_weight,
    down_weight,
):
    z, x = lax.axis_index("z"), lax.axis_index("x")
    y, core = lax.axis_index("y"), lax.axis_index("c")
    kinds = tile_kinds(z, x)
    queries = jnp.concatenate([query_small, query_large], axis=1)
    kv = packed_keys(key_small, value_small, offset_small, key_large, value_large, offset_large)
    kv, queries = lax.optimization_barrier((kv, queries))
    kv_before = lax.ppermute(kv, "z", ring(1))
    kv_after = lax.ppermute(kv, "z", ring(3))
    queries = lax.ppermute(queries, SP, balanced(False))
    q_before = lax.ppermute(queries, "x", ring(1))
    q_after = lax.ppermute(queries, "x", ring(3))
    w = jnp.concatenate([gate_weight, up_weight, down_weight.T], axis=1)
    q_after, w = lax.optimization_barrier((q_after, w))
    w = lax.all_gather(w, SP, axis=0, tiled=True)
    kv = together(kv, kv_before, kv_after, passed_on(kv_before, kv_after, "z"))
    queries = together(queries, q_before, q_after, passed_on(q_before, q_after, "x"))
    outs_in = jnp.concatenate([out_small, out_large], axis=0)
    o_before = lax.ppermute(outs_in, "y", ring(1))
    o_after = lax.ppermute(outs_in, "y", ring(3))
    offsets = kv[:, BLOCK : BLOCK + 6].reshape(4, 3, 4, LANES).astype(jnp.float32) * LOG2E

    outs, totals = attention(kinds, queries, kv, offsets)
    outs, totals, o_before, o_after, residual = lax.optimization_barrier(
        (outs, totals, o_before, o_after, residual)
    )
    r_before = lax.ppermute(residual, "y", ring(1))
    r_after = lax.ppermute(residual, "y", ring(3))
    o_opposite = passed_on(o_before, o_after, "y")
    o_own = together(outs_in, o_before, o_after, o_opposite).reshape(1024, 2048)
    from_before = lax.ppermute(totals, "x", ring(1))
    from_after = lax.ppermute(totals, "x", ring(3))
    from_opposite = lax.ppermute(totals, "x", ring(2))
    spot = jnp.stack([z, x]).astype(jnp.int32)
    o_other = swapped(o_own)
    r_opposite = passed_on(r_before, r_after, "y")
    r_own = together(residual, r_before, r_after, r_opposite)
    r_other = swapped(r_own)
    part = combine(spot, outs, (totals, from_after, from_opposite, from_before))
    mixed = exchanged(part, "x").astype(jnp.bfloat16)
    mixed = lax.ppermute(mixed, SP, balanced(True))
    m_own = ring_gather(mixed, "y", 1)
    m_other = swapped(m_own)
    place = jnp.stack([y, core]).astype(jnp.int32)
    stream, mine, theirs = mlp(
        place, m_own, m_other, r_own, r_other, norm_gain.reshape(1, -1), o_own, o_other, w
    )
    f32 = jnp.float32
    pair = (mine.astype(f32) + swapped(theirs).astype(f32)).astype(jnp.bfloat16)
    summed = exchanged(pair, "y")
    return (stream + summed.astype(jnp.bfloat16).astype(f32)).astype(jnp.bfloat16)


def solution(mesh):
    named = Mesh(mesh.devices.reshape(4, 4, 4, 2), SP + TP)

    return jax.shard_map(
        on_device,
        mesh=named,
        in_specs=(
            P(SP, TP),
            P(SP, TP),
            P(SP, TP),
            P(TP, SP),
            P(SP, TP),
            P(SP, TP),
            P(SP, TP),
            P(TP, SP),
            P(TP, None),
            P(TP, None),
            P(SP + TP, None),
            P(),
            P(SP, TP),
            P(SP, TP),
            P(TP, SP),
        ),
        out_specs=P(SP + TP, None),
        check_vma=False,
    )
```
